32 devices in a mesh: ep: 4 (over y, x), tp: 8 (over z, core).
Axes of the slice: x: 2, y: 2, z: 4, core: 2. Of those that a mesh axis runs over, the one named last changes fastest.
Arguments:
- queries: bfloat16 [4096, 1024], P('ep', 'tp'), may hold values from -8 to 8
- keys: bfloat16 [4096, 256], P('ep'), may hold values from -8 to 8
- values: bfloat16 [4096, 256], P('ep'), may hold values from -6 to 6
- query_gain: float32 [64], replicated, may hold values from 1 to 10
- key_gain: float32 [64], replicated, may hold values from 1 to 10
- moe_input: bfloat16 [1536, 2048], P(('ep', 'tp')), may hold values from -6 to 6
- expert_ids: int32 [1536, 2], P('ep'), may hold values from 0 to 3, all different within a row; in each aligned block of 48 rows (0 to 47, 48 to 95, ...) at most 30 rows name the same one
- route_weight: float32 [1536, 2], P('ep'), may hold values from 0.2 to 1
- gate_weight: bfloat16 [4, 2048, 7168], P('ep', None, 'tp'), may hold values from -0.125 to 0.125
- up_weight: bfloat16 [4, 2048, 7168], P('ep', None, 'tp'), may hold values from -0.125 to 0.125
- down_weight: bfloat16 [4, 7168, 2048], P('ep', 'tp'), may hold values from -0.0625 to 0.0625
- output_gain: float32 [2048], replicated, may hold values from 0.1 to 1.9
Outputs:
- attended: bfloat16 [4096, 1024], P('ep', 'tp')
- moe_output: bfloat16 [1536, 2048], P(('ep', 'tp'))
The draws below stay inside these ranges and needn't reach their ends.
Inputs may be any that keep to these rules, and one draw needn't show every extreme that they name: `expert_ids`: the 2 experts of a token differ. In the rows of one device (aligned blocks of 48 tokens) no expert is named by more than 30 tokens, and in every draw some expert is named by exactly 30 tokens of some device.
All inputs are finite; a program needn't handle non-finite values.
Results may differ from the reference program's by a relative error of at most 0.0085.
The reference program's roundings to bfloat16 on the way count: a program that leaves them out, or rounds other values in their place, can miss the bound.
Values may be sent and summed in bfloat16 or wider, within the bound.
A program may use at most 128 MiB of HBM per device.

```python
import math
import jax
import jax.numpy as jnp
import numpy as np
from jax import lax

D = 2048
HD = 64
QH = 16
KV = 4
GRID_W = 64
H_E = 7168
TOPK = 2
TOK_DEV = 48
LEN = 4096
TOKENS_B = 1536
EXPERTS = 4
CAP = 30
N_EP = 4
N_TP = 8


def draw_keys(key, part):
    normals = jax.random.normal(jax.random.fold_in(key, 31), (LEN, KV * HD), jnp.float32)
    return jnp.clip(normals, -8.0, 8.0).astype(jnp.bfloat16)


def draw_queries(key, part):
    normals = jax.random.normal(jax.random.fold_in(key, 33), (LEN, QH * HD), jnp.float32)
    return jnp.clip(normals, -8.0, 8.0).astype(jnp.bfloat16)


def draw_query_gain(key, part):
    seed_key = jax.random.fold_in(key, 41)
    return jnp.exp(jax.random.uniform(seed_key, (HD,), jnp.float32, 0.0, math.log(2.2)))


def draw_key_gain(key, part):
    seed_key = jax.random.fold_in(key, 43)
    return jnp.exp(jax.random.uniform(seed_key, (HD,), jnp.float32, 0.0, math.log(2.2)))


def block_levels(rng, shape, shards, low, largest):
    loudness = 1.0
    for dim, parts in shards:
        steps = jax.random.uniform(jax.random.fold_in(jax.random.fold_in(rng, 6), dim), (parts,), jnp.float32, low / len(shards), largest / len(shards))
        loudness = loudness * jnp.repeat(jnp.exp(steps), shape[dim] // parts).reshape((-1,) + (1,) * (len(shape) - 1 - dim))
    return loudness


def assign_block(key, own, number, rows, count, top, limit, slope):
    sequence = jax.random.permutation(key, count)
    heavy_load, usual = portions_of(count, rows * top, limit, slope, True), portions_of(count, rows * top, limit, slope, False)
    places = jnp.arange(count)

    def named(tallies, turn):
        used = int((tallies > 0).sum())
        fixed = max(1, used // 4)
        moved = fixed + (places - fixed + turn * (used - fixed)) % max(1, count - fixed)
        return jnp.zeros((count,), jnp.int32).at[sequence[jnp.where(places < fixed, places, moved)]].set(jnp.asarray(tallies, jnp.int32))

    tallies = jnp.where(number % 4 == 0, named(heavy_load, number // 4), named(usual, number - number // 4 - 1))
    mixed = jax.random.permutation(jax.random.fold_in(own, 3), count)
    source_of, sink = mixed[0:count // 2 * 2:2], mixed[1:count // 2 * 2:2]
    room = jnp.minimum(tallies[source_of] - 1, limit - tallies[sink]) // 2
    room = jnp.where((source_of == sequence[0]) | (sink == sequence[0]) | (tallies[sink] == 0), 0, jnp.maximum(room, 0))
    moved = jax.random.randint(jax.random.fold_in(own, 4), (count // 2,), 0, 1 << 20) % (room + 1)
    tallies = tallies.at[source_of].add(-moved).at[sink].add(moved)
    labels = jnp.searchsorted(jnp.cumsum(tallies), jnp.arange(rows * top), side="right").astype(jnp.int32)
    table = labels.reshape(top, rows).T
    table = table[jax.random.permutation(jax.random.fold_in(own, 1), rows)]
    turn = jax.random.randint(jax.random.fold_in(own, 2), (rows, 1), 0, top)
    return jnp.take_along_axis(table, (jnp.arange(top)[None, :] + turn) % top, axis=1)


def portions_of(number_of, total, limit, skew, full):
    portions = [(1 << 20) // math.isqrt(grade ** skew) + 1 for grade in range(1, number_of + 1)]
    largest = limit if full else min(limit, max(-(-total // number_of), total * portions[0] // sum(portions)))
    least = 1 if total - largest >= number_of - 1 else 0
    counts, spare = [largest] + [least] * (number_of - 1), total - largest - least * (number_of - 1)
    while spare > 0:
        movable = [i for i in range(1, number_of) if counts[i] < largest] or [i for i in range(1, number_of) if counts[i] < limit]
        mass, remaining = sum([portions[i] for i in movable]), spare
        for i in movable:
            addition = min(limit - counts[i], max(1, remaining * portions[i] // mass), spare)
            counts[i] = counts[i] + addition
            spare = spare - addition
    return np.array(counts)


def centred(own_key, dims, scale, reach, shards=(), held_as=jnp.bfloat16):
    level = block_levels(own_key, dims, shards, -0.22, 0.18) if shards else 1.0
    drawn = jax.random.normal(own_key, dims, jnp.float32) * scale * level
    return jnp.minimum(jnp.maximum(drawn, -reach), reach).astype(held_as)


def setup_inputs(seed: int = 0) -> dict:
    seeds = jax.random.split(jax.random.key(seed), 13)
    queries = draw_queries(jax.random.fold_in(seeds[12], 71), 0)
    keys = draw_keys(jax.random.fold_in(seeds[12], 71), 0)
    values = centred(seeds[2], (LEN, KV * HD), 1.0, 6.0, ((0, 4),))
    query_gain = draw_query_gain(jax.random.fold_in(seeds[12], 71), 0)
    key_gain = draw_key_gain(jax.random.fold_in(seeds[12], 71), 0)
    moe_input = centred(seeds[5], (TOKENS_B, D), 1.0, 6.0, ((0, 32),))
    expert_ids_keys = jax.random.split(jax.random.fold_in(seeds[6], 1), TOKENS_B // TOK_DEV)
    expert_ids_turns = jax.random.permutation(jax.random.fold_in(seeds[6], 3), TOKENS_B // TOK_DEV)
    expert_ids = jax.vmap(lambda own, number: assign_block(jax.random.fold_in(seeds[6], 2), own, number, TOK_DEV, EXPERTS, TOPK, CAP, 1))(expert_ids_keys, expert_ids_turns).reshape((TOKENS_B, TOPK))
    route_weight = jnp.clip(0.2 + 0.8 * jax.random.uniform(seeds[7], (TOKENS_B, TOPK), jnp.float32) ** block_levels(seeds[7], (TOKENS_B, TOPK), ((0, 4),), -0.2, 0.2), 0.2, 1.0)
    gate_weight = centred(seeds[8], (EXPERTS, D, H_E), D ** -0.5, 0.125, ((0, 4), (2, 8)))
    up_weight = centred(seeds[9], (EXPERTS, D, H_E), D ** -0.5, 0.125, ((0, 4), (2, 8)))
    down_weight = centred(seeds[10], (EXPERTS, H_E, D), H_E ** -0.5, 0.0625, ((0, 4), (1, 8)))
    output_gain = jnp.clip(1.0 + 0.18 * jax.random.normal(seeds[11], (D,), jnp.float32), 0.1, 1.9)
    return {"queries": queries, "keys": keys, "values": values, "query_gain": query_gain, "key_gain": key_gain, "moe_input": moe_input, "expert_ids": expert_ids, "route_weight": route_weight, "gate_weight": gate_weight, "up_weight": up_weight, "down_weight": down_weight, "output_gain": output_gain}


rope_theta = 10000.0
rms_epsilon = 1e-06
norm_epsilon = 1e-05
residual_scale = 1.4142135623730951

def unit_heads(heads, gain_vector):
    squares = lax.optimization_barrier(jnp.mean(heads * heads, axis=-1, keepdims=True))
    return heads * lax.rsqrt(squares + rms_epsilon) * gain_vector

def rotate_grid(heads, first_position, grid_width):
    head_size = heads.shape[-1]
    pair_count = head_size // 4
    position = first_position + jnp.arange(heads.shape[1], dtype=jnp.int32)
    grid_row = (position // grid_width).astype(jnp.float32)
    grid_col = (position % grid_width).astype(jnp.float32)
    inverse = rope_theta ** (-jnp.arange(pair_count, dtype=jnp.float32) / pair_count)
    angles = jnp.concatenate([grid_row[:, None] * inverse, grid_col[:, None] * inverse], axis=-1)
    cosines = jnp.cos(angles)
    sines = jnp.sin(angles)
    half_size = head_size // 2
    first_half = heads[..., :half_size]
    second_half = heads[..., half_size:]
    return jnp.concatenate([first_half * cosines - second_half * sines, second_half * cosines + first_half * sines], axis=-1)

def place_rank(choices, expert_count):
    matches = (choices[..., None] == jnp.arange(expert_count, dtype=jnp.int32)).astype(jnp.int32)
    earlier = jnp.cumsum(matches, axis=1) - matches
    return lax.optimization_barrier(jnp.sum(earlier * matches, axis=-1)).astype(jnp.int32)

def attention(queries, keys, values, query_gain, key_gain):
    length = queries.shape[0]
    query_heads = queries.reshape(length, QH, HD).transpose(1, 0, 2).astype(jnp.float32)
    rotated_queries = rotate_grid(unit_heads(query_heads, query_gain), 0, GRID_W).astype(jnp.bfloat16)
    key_heads = keys.reshape(length, KV, HD).transpose(1, 0, 2).astype(jnp.float32)
    rotated_keys = rotate_grid(unit_heads(key_heads, key_gain), 0, GRID_W).astype(jnp.bfloat16)
    value_heads = values.reshape(length, KV, HD).transpose(1, 0, 2)
    query_block = math.gcd(length, 1024)
    group_size = QH // KV
    score_scale = HD ** (-0.5)

    def one_head(head_index):
        key_rows = lax.dynamic_index_in_dim(rotated_keys, head_index // group_size, 0, keepdims=False)
        value_rows = lax.dynamic_index_in_dim(value_heads, head_index // group_size, 0, keepdims=False)
        query_rows = lax.dynamic_index_in_dim(rotated_queries, head_index, 0, keepdims=False)

        def one_block(query_part):
            scores = jnp.dot(query_part, key_rows.T, preferred_element_type=jnp.float32) * score_scale
            row_max = lax.optimization_barrier(jnp.max(scores, axis=-1, keepdims=True))
            weights = jnp.exp(scores - row_max)
            totals = lax.optimization_barrier(jnp.sum(weights, axis=-1, keepdims=True))
            summed = jnp.dot(weights.astype(jnp.bfloat16), value_rows, preferred_element_type=jnp.float32)
            return (summed / totals).astype(jnp.bfloat16)
        blocks = query_rows.reshape(length // query_block, query_block, HD)
        return lax.map(one_block, blocks).reshape(length, HD)
    attended = lax.map(one_head, jnp.arange(QH, dtype=jnp.int32))
    return attended.transpose(1, 0, 2).reshape(length, QH * HD)

def run_expert(operands):
    expert_rows, gate_matrix, up_matrix, down_matrix = operands
    gate_part = jnp.dot(expert_rows, gate_matrix, preferred_element_type=jnp.float32)
    up_part = jnp.dot(expert_rows, up_matrix, preferred_element_type=jnp.float32)
    hidden = (jax.nn.silu(gate_part) * up_part).astype(jnp.bfloat16)
    group_width = hidden.shape[1] // N_TP
    hidden_groups = hidden.reshape(hidden.shape[0], N_TP, group_width).transpose(1, 0, 2)
    down_groups = down_matrix.reshape(N_TP, group_width, down_matrix.shape[1])

    def add_group(running, operand_pair):
        hidden_part, down_part = operand_pair
        partial_sum = jnp.dot(hidden_part, down_part, preferred_element_type=jnp.float32)
        rounded = lax.optimization_barrier(partial_sum.astype(jnp.bfloat16))
        return (running + rounded.astype(jnp.float32), None)
    start_sum = jnp.zeros((hidden.shape[0], down_matrix.shape[1]), jnp.float32)
    summed, ignored = lax.scan(add_group, start_sum, (hidden_groups, down_groups))
    return summed.astype(jnp.bfloat16)

def layer_scale(mixed, gain_vector):
    average = lax.optimization_barrier(jnp.mean(mixed, axis=-1, keepdims=True))
    centered = mixed - average
    variance = lax.optimization_barrier(jnp.mean(centered * centered, axis=-1, keepdims=True))
    return (centered * lax.rsqrt(variance + norm_epsilon) * gain_vector).astype(jnp.bfloat16)

def experts_layer(moe_input, expert_ids, route_weight, gate_weight, up_weight, down_weight, output_gain):
    top_count = expert_ids.shape[1]
    block_count = N_EP * N_TP
    choices = expert_ids.reshape(block_count, TOK_DEV * top_count)
    ranks = place_rank(choices, EXPERTS)
    expert_span = block_count * CAP
    targets = choices * expert_span + jnp.arange(block_count, dtype=jnp.int32)[:, None] * CAP + ranks
    tokens_from = jnp.arange(block_count * TOK_DEV * top_count, dtype=jnp.int32) // top_count
    sources = jnp.full((EXPERTS * expert_span,), block_count * TOK_DEV, jnp.int32).at[targets.reshape(-1)].set(tokens_from)
    gathered = jnp.take(moe_input, sources, axis=0, mode='fill', fill_value=0).reshape(EXPERTS, expert_span, D)
    outputs = lax.map(run_expert, (gathered, gate_weight, up_weight, down_weight))
    picked = jnp.take(outputs.reshape(EXPERTS * expert_span, D), targets.reshape(-1), axis=0)
    picked = picked.reshape(block_count * TOK_DEV, top_count, D).astype(jnp.float32)
    mixed = residual_scale * moe_input.astype(jnp.float32) + lax.optimization_barrier(jnp.sum(route_weight[:, :, None] * picked, axis=1))
    return layer_scale(mixed, output_gain)

def reference(queries, keys, values, query_gain, key_gain, moe_input, expert_ids, route_weight, gate_weight, up_weight, down_weight, output_gain):
    attended = attention(queries, keys, values, query_gain, key_gain)
    moe_output = experts_layer(moe_input, expert_ids, route_weight, gate_weight, up_weight, down_weight, output_gain)
    return (attended, moe_output)
```

```python
import math

import jax
import jax.numpy as jnp
from jax import lax
from jax.experimental import pallas as pl
from jax.experimental.pallas import tpu as pltpu
from jax.sharding import PartitionSpec as P

QH = 16
KV = 4
GRID_W = 64


rope_theta = 10000.0
rms_epsilon = 1e-06
norm_epsilon = 1e-05
residual_scale = 1.4142135623730951


def unit_heads(heads, gain_vector):
    squares = jnp.mean(heads * heads, axis=-1, keepdims=True)
    return heads * lax.rsqrt(squares + rms_epsilon) * gain_vector


def rotate_grid(heads, first_position, grid_width):
    head_size = heads.shape[-1]
    pair_count = head_size // 4
    position = first_position + jnp.arange(heads.shape[1], dtype=jnp.int32)
    grid_row = (position // grid_width).astype(jnp.float32)
    grid_col = (position % grid_width).astype(jnp.float32)
    inverse = rope_theta ** (-jnp.arange(pair_count, dtype=jnp.float32) / pair_count)
    angles = jnp.concatenate([grid_row[:, None] * inverse, grid_col[:, None] * inverse], axis=-1)
    cosines = jnp.cos(angles)
    sines = jnp.sin(angles)
    half_size = head_size // 2
    first_half = heads[..., :half_size]
    second_half = heads[..., half_size:]
    return jnp.concatenate(
        [first_half * cosines - second_half * sines, second_half * cosines + first_half * sines],
        axis=-1,
    )


def round_up(value, multiple):
    return -(-value // multiple) * multiple


def attention_body(q_ref, kv_ref, out_ref, *, head_size):
    parts = []
    for head in range(q_ref.shape[0]):
        scores = lax.dot_general(
            q_ref[head], kv_ref[...], (((1,), (1,)), ((), ())), preferred_element_type=jnp.float32
        )
        weights = jnp.exp(scores - jnp.max(scores, axis=-1, keepdims=True))
        total = jnp.sum(weights, axis=-1, keepdims=True)
        summed = jnp.dot(
            weights.astype(jnp.bfloat16), kv_ref[...], preferred_element_type=jnp.float32
        )
        parts.append(summed[:, :head_size] / total)
    out_ref[...] = jnp.concatenate(parts, axis=-1).astype(out_ref.dtype)


def attend(padded_queries, key_values, head_size):
    heads, rows, width = padded_queries.shape
    length = key_values.shape[0]
    block = math.gcd(rows, 128)
    return pl.pallas_call(
        lambda *refs: attention_body(*refs, head_size=head_size),
        grid=(rows // block,),
        in_specs=[
            pl.BlockSpec((heads, block, width), lambda i: (0, i, 0)),
            pl.BlockSpec((length, width), lambda i: (0, 0)),
        ],
        out_specs=pl.BlockSpec((block, heads * head_size), lambda i: (i, 0)),
        out_shape=jax.ShapeDtypeStruct((rows, heads * head_size), jnp.bfloat16),
        compiler_params=pltpu.CompilerParams(vmem_limit_bytes=40 * 1024 * 1024),
        cost_estimate=pl.CostEstimate(
            flops=16 * heads * rows * length * head_size,
            bytes_accessed=2 * width * (heads * rows + length),
            transcendentals=heads * rows * length,
        ),
    )(padded_queries, key_values)


def shards(
    queries,
    keys,
    values,
    query_gain,
    key_gain,
    moe_input,
    expert_ids,
    route_weight,
    gate_weight,
    up_weight,
    down_weight,
    output_gain,
):
    n_ep = lax.axis_size("ep")
    n_tp = lax.axis_size("tp")
    n_z = n_tp // 2
    ep_index = lax.axis_index("ep")
    tp_index = lax.axis_index("tp")

    def across(array, step):
        return lax.ppermute(array, "ep", [(i, i ^ step) for i in range(n_ep)])

    def partner(array):
        return lax.ppermute(array, "tp", [(i, i ^ 1) for i in range(n_tp)])

    def shift(array, chips):
        return lax.ppermute(array, "tp", [(i, (i + 2 * chips) % n_tp) for i in range(n_tp)])

    def add(first, second):
        return (first.astype(jnp.float32) + second.astype(jnp.float32)).astype(jnp.bfloat16)

    tok_rows, model_width = moe_input.shape
    top_count = expert_ids.shape[1]
    capacity = round_up(max(2, tok_rows * top_count * 5 // (4 * n_ep)), 16)
    slot_count = n_ep * capacity
    own_ids = lax.dynamic_slice_in_dim(expert_ids, tp_index * tok_rows, tok_rows, 0)
    own_weights = lax.dynamic_slice_in_dim(route_weight, tp_index * tok_rows, tok_rows, 0)
    flat_ids = own_ids.reshape(-1)
    order = jnp.arange(tok_rows * top_count, dtype=jnp.int32)
    earlier = (flat_ids[:, None] == flat_ids[None, :]) & (order[None, :] < order[:, None])
    rank = jnp.sum(earlier.astype(jnp.int32), axis=1)
    slots = ((flat_ids ^ ep_index) * capacity + rank).reshape(tok_rows, top_count)
    slot_index = jnp.arange(slot_count, dtype=jnp.int32)
    chosen = slots[:, :, None] == slot_index
    named = jnp.any(chosen, axis=1).astype(jnp.bfloat16)
    outgoing = lax.dot_general(
        named, moe_input, (((0,), (0,)), ((), ())), preferred_element_type=jnp.float32
    ).astype(jnp.bfloat16)
    outgoing = outgoing.reshape(n_ep, capacity, model_width)

    seg_rows = queries.shape[0]
    head_size = query_gain.shape[0]
    local_heads = queries.shape[1] // head_size
    offset = ep_index * seg_rows
    half_rows = seg_rows // 2
    core = lax.rem(tp_index, 2)
    key_head = tp_index * local_heads // (QH // KV)
    first_row = core * half_rows
    key_cols = lax.dynamic_slice(
        keys, (first_row, key_head * head_size), (half_rows, head_size)
    )
    value_cols = lax.dynamic_slice(
        values, (first_row, key_head * head_size), (half_rows, head_size)
    )
    key_heads = key_cols.astype(jnp.float32)[None]
    rotated_keys = rotate_grid(unit_heads(key_heads, key_gain), offset + first_row, GRID_W)[
        0
    ].astype(jnp.bfloat16)
    own_kv = jnp.concatenate([value_cols, rotated_keys], axis=-1)

    kv_pieces = [own_kv] + [across(own_kv, step) for step in range(1, n_ep)]
    slab = jnp.concatenate(
        [outgoing[0]] + [across(outgoing[step], step) for step in range(1, n_ep)], axis=0
    )

    kv_half = jnp.concatenate(kv_pieces, axis=0)
    key_values = jnp.concatenate([kv_half, partner(kv_half)], axis=0)
    query_heads = (
        queries.reshape(seg_rows, local_heads, head_size).transpose(1, 0, 2).astype(jnp.float32)
    )
    rotated_queries = rotate_grid(unit_heads(query_heads, query_gain), offset, GRID_W).astype(
        jnp.bfloat16
    ) * jnp.bfloat16(head_size ** (-0.5))
    padded_queries = jnp.concatenate(
        [jnp.zeros_like(rotated_queries), rotated_queries], axis=-1
    )
    attended = attend(padded_queries, key_values, head_size)

    slab_rows = slab.shape[0]
    half_slab = slab_rows // 2
    reach = n_z // 2
    ahead, behind = [slab], [slab]
    for distance in range(1, reach):
        ahead.append(shift(ahead[-1], 1))
        behind.append(shift(behind[-1], -1))
    last = jnp.concatenate(
        [shift(ahead[-1][:half_slab], 1), shift(behind[-1][half_slab:], -1)], axis=0
    )
    mine = [slab] + ahead[1:] + behind[1:] + [last]
    theirs = [partner(piece) for piece in mine]
    rows = jnp.concatenate(mine + theirs, axis=0)

    gate_part = jnp.dot(rows, gate_weight[0], preferred_element_type=jnp.float32)
    up_part = jnp.dot(rows, up_weight[0], preferred_element_type=jnp.float32)
    hidden = (jax.nn.silu(gate_part) * up_part).astype(jnp.bfloat16)
    own_count = n_z * slab_rows
    sent = jnp.dot(hidden[own_count:], down_weight[0], preferred_element_type=jnp.float32)
    from_partner = partner(sent.astype(jnp.bfloat16))
    kept = jnp.dot(hidden[:own_count], down_weight[0], preferred_element_type=jnp.float32)
    sums = add(kept.astype(jnp.bfloat16), from_partner).reshape(n_z, slab_rows, model_width)
    behind_of = {0: sums[0]} | {d: sums[d] for d in range(1, reach)}
    ahead_of = {0: sums[0]} | {d: sums[reach - 1 + d] for d in range(1, reach)}
    far = sums[n_z - 1]
    right, left = far[:half_slab], far[half_slab:]
    for distance in range(reach - 1, 0, -1):
        came_right, came_left = shift(right, 1), shift(left, -1)
        onward, back = ahead_of[distance], behind_of[distance]
        if distance == reach - 1:
            right = jnp.concatenate([add(onward[:half_slab], came_right), onward[half_slab:]], 0)
            left = jnp.concatenate([back[:half_slab], add(back[half_slab:], came_left)], 0)
        else:
            right, left = add(onward, came_right), add(back, came_left)
    came_right, came_left = shift(right, 1), shift(left, -1)
    if reach == 1:
        expert_out = add(sums[0], jnp.concatenate([came_right, came_left], 0))
    else:
        expert_out = (
            sums[0].astype(jnp.float32)
            + came_right.astype(jnp.float32)
            + came_left.astype(jnp.float32)
        ).astype(jnp.bfloat16)
    expert_out = expert_out.reshape(n_ep, capacity, model_width)
    returned = jnp.concatenate(
        [expert_out[0]] + [across(expert_out[step], step) for step in range(1, n_ep)], axis=0
    )
    mixed = residual_scale * moe_input.astype(jnp.float32)
    for k in range(top_count):
        picked = jnp.dot(
            chosen[:, k].astype(jnp.bfloat16), returned, preferred_element_type=jnp.float32
        )
        mixed = mixed + own_weights[:, k : k + 1] * picked
    average = jnp.mean(mixed, axis=-1, keepdims=True)
    centered = mixed - average
    variance = jnp.mean(centered * centered, axis=-1, keepdims=True)
    moe_output = (centered * lax.rsqrt(variance + norm_epsilon) * output_gain).astype(jnp.bfloat16)
    return (attended, moe_output)


def solution(mesh):
    in_specs = (
        P("ep", "tp"),
        P("ep", None),
        P("ep", None),
        P(),
        P(),
        P(("ep", "tp"), None),
        P("ep", None),
        P("ep", None),
        P("ep", None, "tp"),
        P("ep", None, "tp"),
        P("ep", "tp", None),
        P(),
    )
    out_specs = (P("ep", "tp"), P(("ep", "tp"), None))
    return jax.shard_map(shards, mesh=mesh, in_specs=in_specs, out_specs=out_specs, check_vma=False)
```

```python
import math

import jax
import jax.numpy as jnp
from jax import lax
from jax.experimental import pallas as pl
from jax.experimental.pallas import tpu as pltpu
from jax.sharding import PartitionSpec as P

QH = 16
KV = 4
GRID_W = 64


rope_theta = 10000.0
rms_epsilon = 1e-06
norm_epsilon = 1e-05
residual_scale = 1.4142135623730951


def unit_heads(heads, gain_vector):
    squares = jnp.mean(heads * heads, axis=-1, keepdims=True)
    return heads * lax.rsqrt(squares + rms_epsilon) * gain_vector


def rotate_grid(heads, first_position, grid_width):
    head_size = heads.shape[-1]
    pair_count = head_size // 4
    position = first_position + jnp.arange(heads.shape[1], dtype=jnp.int32)
    grid_row = (position // grid_width).astype(jnp.float32)
    grid_col = (position % grid_width).astype(jnp.float32)
    inverse = rope_theta ** (-jnp.arange(pair_count, dtype=jnp.float32) / pair_count)
    angles = jnp.concatenate([grid_row[:, None] * inverse, grid_col[:, None] * inverse], axis=-1)
    cosines = jnp.cos(angles)
    sines = jnp.sin(angles)
    half_size = head_size // 2
    first_half = heads[..., :half_size]
    second_half = heads[..., half_size:]
    return jnp.concatenate(
        [first_half * cosines - second_half * sines, second_half * cosines + first_half * sines],
        axis=-1,
    )


def round_up(value, multiple):
    return -(-value // multiple) * multiple


def attention_body(q_ref, kv_ref, out_ref, *, head_size):
    parts = []
    for head in range(q_ref.shape[0]):
        scores = lax.dot_general(
            q_ref[head], kv_ref[...], (((1,), (1,)), ((), ())), preferred_element_type=jnp.float32
        )
        weights = jnp.exp(scores - jnp.max(scores, axis=-1, keepdims=True))
        total = jnp.sum(weights, axis=-1, keepdims=True)
        summed = jnp.dot(
            weights.astype(jnp.bfloat16), kv_ref[...], preferred_element_type=jnp.float32
        )
        parts.append(summed[:, :head_size] / total)
    out_ref[...] = jnp.concatenate(parts, axis=-1).astype(out_ref.dtype)


def attend(padded_queries, key_values, head_size):
    heads, rows, width = padded_queries.shape
    length = key_values.shape[0]
    block = math.gcd(rows, 128)
    return pl.pallas_call(
        lambda *refs: attention_body(*refs, head_size=head_size),
        grid=(rows // block,),
        in_specs=[
            pl.BlockSpec((heads, block, width), lambda i: (0, i, 0)),
            pl.BlockSpec((length, width), lambda i: (0, 0)),
        ],
        out_specs=pl.BlockSpec((block, heads * head_size), lambda i: (i, 0)),
        out_shape=jax.ShapeDtypeStruct((rows, heads * head_size), jnp.bfloat16),
        compiler_params=pltpu.CompilerParams(vmem_limit_bytes=40 * 1024 * 1024),
        cost_estimate=pl.CostEstimate(
            flops=16 * heads * rows * length * head_size,
            bytes_accessed=2 * width * (heads * rows + length),
            transcendentals=heads * rows * length,
        ),
    )(padded_queries, key_values)


def hidden_body(*refs, starts, width):
    pieces, (gate_ref, up_ref, out_ref, rows_ref) = refs[: len(starts)], refs[len(starts) :]

    @pl.when(pl.program_id(0) == 0)
    def assemble():
        for start, piece in zip(starts, pieces):
            rows_ref[start : start + piece.shape[0], :] = piece[...]

    both = jnp.dot(
        rows_ref[...],
        jnp.concatenate([gate_ref[0], up_ref[0]], axis=1),
        preferred_element_type=jnp.float32,
    )
    out_ref[...] = (jax.nn.silu(both[:, :width]) * both[:, width:]).astype(out_ref.dtype)


def expert_hidden(pieces, gate_weight, up_weight):
    model_width, units = gate_weight.shape[1:]
    starts, total = [], 0
    for piece in pieces:
        starts.append(total)
        total += piece.shape[0]
    if units % 128 or total * model_width > 1 << 22:
        rows = jnp.concatenate(pieces, axis=0)
        gate_part = jnp.dot(rows, gate_weight[0], preferred_element_type=jnp.float32)
        up_part = jnp.dot(rows, up_weight[0], preferred_element_type=jnp.float32)
        return (jax.nn.silu(gate_part) * up_part).astype(jnp.bfloat16)
    width = 128
    weight_spec = pl.BlockSpec((1, model_width, width), lambda i: (0, 0, i))
    return pl.pallas_call(
        lambda *refs: hidden_body(*refs, starts=starts, width=width),
        grid=(units // width,),
        in_specs=[pl.BlockSpec(piece.shape, lambda i: (0, 0)) for piece in pieces]
        + [weight_spec, weight_spec],
        out_specs=pl.BlockSpec((total, width), lambda i: (0, i)),
        out_shape=jax.ShapeDtypeStruct((total, units), jnp.bfloat16),
        scratch_shapes=[pltpu.VMEM((total, model_width), jnp.bfloat16)],
        compiler_params=pltpu.CompilerParams(vmem_limit_bytes=40 * 1024 * 1024),
        cost_estimate=pl.CostEstimate(
            flops=4 * total * model_width * units,
            bytes_accessed=2 * model_width * (total + 2 * units),
            transcendentals=total * units,
        ),
    )(*pieces, gate_weight, up_weight)


def shards(
    queries,
    keys,
    values,
    query_gain,
    key_gain,
    moe_input,
    expert_ids,
    route_weight,
    gate_weight,
    up_weight,
    down_weight,
    output_gain,
):
    n_ep = lax.axis_size("ep")
    n_tp = lax.axis_size("tp")
    n_z = n_tp // 2
    ep_index = lax.axis_index("ep")
    tp_index = lax.axis_index("tp")

    def across(array, step):
        return lax.ppermute(array, "ep", [(i, i ^ step) for i in range(n_ep)])

    def partner(array):
        return lax.ppermute(array, "tp", [(i, i ^ 1) for i in range(n_tp)])

    def shift(array, chips):
        return lax.ppermute(array, "tp", [(i, (i + 2 * chips) % n_tp) for i in range(n_tp)])

    def add(first, second):
        return (first.astype(jnp.float32) + second.astype(jnp.float32)).astype(jnp.bfloat16)

    tok_rows, model_width = moe_input.shape
    top_count = expert_ids.shape[1]
    capacity = round_up(max(2, tok_rows * top_count * 5 // (4 * n_ep)), 16)
    slot_count = n_ep * capacity
    own_ids = lax.dynamic_slice_in_dim(expert_ids, tp_index * tok_rows, tok_rows, 0)
    own_weights = lax.dynamic_slice_in_dim(route_weight, tp_index * tok_rows, tok_rows, 0)
    flat_ids = own_ids.reshape(-1)
    order = jnp.arange(tok_rows * top_count, dtype=jnp.int32)
    earlier = (flat_ids[:, None] == flat_ids[None, :]) & (order[None, :] < order[:, None])
    rank = jnp.sum(earlier.astype(jnp.int32), axis=1)
    slots = ((flat_ids ^ ep_index) * capacity + rank).reshape(tok_rows, top_count)
    slot_index = jnp.arange(slot_count, dtype=jnp.int32)
    chosen = slots[:, :, None] == slot_index
    named = jnp.any(chosen, axis=1).astype(jnp.bfloat16)
    outgoing = lax.dot_general(
        named, moe_input, (((0,), (0,)), ((), ())), preferred_element_type=jnp.float32
    ).astype(jnp.bfloat16)
    outgoing = outgoing.reshape(n_ep, capacity, model_width)

    outgoing, keys, values, queries = lax.optimization_barrier((outgoing, keys, values, queries))

    seg_rows = queries.shape[0]
    head_size = query_gain.shape[0]
    local_heads = queries.shape[1] // head_size
    offset = ep_index * seg_rows
    half_rows = seg_rows // 2
    core = lax.rem(tp_index, 2)
    key_head = tp_index * local_heads // (QH // KV)
    first_row = core * half_rows
    key_cols = lax.dynamic_slice(
        keys, (first_row, key_head * head_size), (half_rows, head_size)
    )
    value_cols = lax.dynamic_slice(
        values, (first_row, key_head * head_size), (half_rows, head_size)
    )
    key_heads = key_cols.astype(jnp.float32)[None]
    rotated_keys = rotate_grid(unit_heads(key_heads, key_gain), offset + first_row, GRID_W)[
        0
    ].astype(jnp.bfloat16)
    own_kv = jnp.concatenate([value_cols, rotated_keys], axis=-1)

    kv_pieces = [own_kv] + [across(own_kv, step) for step in range(1, n_ep)]
    slab = jnp.concatenate(
        [outgoing[0]] + [across(outgoing[step], step) for step in range(1, n_ep)], axis=0
    )

    kv_half = jnp.concatenate(kv_pieces, axis=0)
    query_heads = (
        queries.reshape(seg_rows, local_heads, head_size).transpose(1, 0, 2).astype(jnp.float32)
    )
    rotated_queries = rotate_grid(unit_heads(query_heads, query_gain), offset, GRID_W).astype(
        jnp.bfloat16
    ) * jnp.bfloat16(head_size ** (-0.5))
    padded_queries = jnp.concatenate(
        [jnp.zeros_like(rotated_queries), rotated_queries], axis=-1
    )

    slab_rows = slab.shape[0]
    half_slab = slab_rows // 2
    reach = n_z // 2
    ahead, behind = [slab], [slab]
    for distance in range(1, reach):
        ahead.append(shift(ahead[-1], 1))
        behind.append(shift(behind[-1], -1))
    ahead[-1], behind[-1], kv_half, padded_queries = lax.optimization_barrier(
        (ahead[-1], behind[-1], kv_half, padded_queries)
    )
    key_values = jnp.concatenate([kv_half, partner(kv_half)], axis=0)
    last = [shift(ahead[-1][:half_slab], 1), shift(behind[-1][half_slab:], -1)]
    mine = [slab] + ahead[1:] + behind[1:] + last
    theirs = [partner(piece) for piece in mine]
    *pieces, key_values = lax.optimization_barrier((*mine, *theirs, key_values))
    hidden = expert_hidden(pieces, gate_weight, up_weight)
    own_count = n_z * slab_rows
    sent = jnp.dot(hidden[own_count:], down_weight[0], preferred_element_type=jnp.float32)
    from_partner = partner(sent.astype(jnp.bfloat16))
    kept = jnp.dot(hidden[:own_count], down_weight[0], preferred_element_type=jnp.float32)
    kept = lax.optimization_barrier(kept.astype(jnp.bfloat16))
    sums = add(kept, from_partner).reshape(n_z, slab_rows, model_width)
    behind_of = {0: sums[0]} | {d: sums[d] for d in range(1, reach)}
    ahead_of = {0: sums[0]} | {d: sums[reach - 1 + d] for d in range(1, reach)}
    far = sums[n_z - 1]
    right, left = far[:half_slab], far[half_slab:]
    for distance in range(reach - 1, 0, -1):
        came_right, came_left = shift(right, 1), shift(left, -1)
        onward, back = ahead_of[distance], behind_of[distance]
        if distance == reach - 1:
            right = jnp.concatenate([add(onward[:half_slab], came_right), onward[half_slab:]], 0)
            left = jnp.concatenate([back[:half_slab], add(back[half_slab:], came_left)], 0)
        else:
            right, left = add(onward, came_right), add(back, came_left)
    came_right, came_left = shift(right, 1), shift(left, -1)
    attended = attend(padded_queries, key_values, head_size)
    came_right, came_left, attended = lax.optimization_barrier((came_right, came_left, attended))
    if reach == 1:
        expert_out = add(sums[0], jnp.concatenate([came_right, came_left], 0))
    else:
        expert_out = (
            sums[0].astype(jnp.float32)
            + came_right.astype(jnp.float32)
            + came_left.astype(jnp.float32)
        ).astype(jnp.bfloat16)
    expert_out = expert_out.reshape(n_ep, capacity, model_width)
    returned = jnp.concatenate(
        [expert_out[0]] + [across(expert_out[step], step) for step in range(1, n_ep)], axis=0
    )
    mixed = residual_scale * moe_input.astype(jnp.float32)
    for k in range(top_count):
        picked = jnp.dot(
            chosen[:, k].astype(jnp.bfloat16), returned, preferred_element_type=jnp.float32
        )
        mixed = mixed + own_weights[:, k : k + 1] * picked
    average = jnp.mean(mixed, axis=-1, keepdims=True)
    centered = mixed - average
    variance = jnp.mean(centered * centered, axis=-1, keepdims=True)
    moe_output = (centered * lax.rsqrt(variance + norm_epsilon) * output_gain).astype(jnp.bfloat16)
    return (attended, moe_output)


def solution(mesh):
    in_specs = (
        P("ep", "tp"),
        P("ep", None),
        P("ep", None),
        P(),
        P(),
        P(("ep", "tp"), None),
        P("ep", None),
        P("ep", None),
        P("ep", None, "tp"),
        P("ep", None, "tp"),
        P("ep", "tp", None),
        P(),
    )
    out_specs = (P("ep", "tp"), P(("ep", "tp"), None))
    return jax.shard_map(shards, mesh=mesh, in_specs=in_specs, out_specs=out_specs, check_vma=False)
```
